32 devices in a mesh: sp: 8 (over z, y), tp: 4 (over x, core).
Axes of the slice: x: 2, y: 2, z: 4, core: 2. Of those that a mesh axis runs over, the one named last changes fastest.
Arguments:
- resid: bfloat16 [2048, 2048], P(('sp', 'tp')), may hold values from -6 to 6
- query_a: bfloat16 [2048, 4, 128], P('sp', 'tp')
- key_a: bfloat16 [2048, 4, 128], P('sp', 'tp')
- value_a: bfloat16 [2048, 4, 128], P('sp', 'tp'), may hold values from -6 to 6
- query_b: bfloat16 [2048, 4, 256], P('sp', 'tp')
- key_b: bfloat16 [2048, 4, 256], P('sp', 'tp')
- value_b: bfloat16 [2048, 4, 128], P('sp', 'tp'), may hold values from -6 to 6
- lambda_a: float32 [4], P('tp'), may hold values from 0.3 to 0.8
- lambda_b: float32 [4], P('tp'), may hold values from 0.3 to 0.8
- head_gain: float32 [128], replicated, may hold values from 0.1 to 1.9
- out_weight: bfloat16 [1024, 2048], replicated, may hold values from -0.1875 to 0.1875
- norm_gain: float32 [2048], replicated, may hold values from 0.1 to 1.9
- expert_ids: int32 [2048, 4], P(('sp', 'tp')), may hold values from 0 to 31, all different within a row; in each aligned block of 64 rows (0 to 63, 64 to 127, ...) at most 16 rows name the same one
- expert_mix: float32 [2048, 4], P(('sp', 'tp')), may hold values from 0.2 to 1
- gate_experts: bfloat16 [32, 2048, 1024], P(('sp', 'tp')), may hold values from -0.125 to 0.125
- up_experts: bfloat16 [32, 2048, 1024], P(('sp', 'tp')), may hold values from -0.125 to 0.125
- down_experts: bfloat16 [32, 1024, 2048], P(('sp', 'tp')), may hold values from -0.1875 to 0.1875
- shared_gate: bfloat16 [2048, 512], replicated, may hold values from -0.125 to 0.125
- shared_up: bfloat16 [2048, 512], replicated, may hold values from -0.125 to 0.125
- shared_down: bfloat16 [512, 2048], replicated, may hold values from -0.25 to 0.25
Outputs:
- layer_out: bfloat16 [2048, 2048], P(('sp', 'tp'))
The draws below stay inside these ranges and needn't reach their ends.
Inputs may be any that keep to these rules, and one draw needn't show every extreme that they name: `expert_ids`: in each aligned block of 64 rows (the rows of one device) no expert is named more than 16 times, a bound that some block reaches.
All inputs are finite; a program needn't handle non-finite values.
Results may differ from the reference program's by a relative error of at most 0.017.
Values may be sent and summed in bfloat16 or wider, within the bound.
A program may use at most 128 MiB of HBM per device.

```python
import math
import jax
import jax.numpy as jnp
import numpy as np
from jax import lax

D = 2048
HA = 4
HB = 4
DA = 64
DB = 128
DV = 128
EFF = 1024
SFF = 512
TOPK = 4
TOK_DEV = 64
TOKENS = 2048
EXPERTS = 32
CAP = 16
N_SP = 8
N_TP = 4


def drawn_pair(key, tag, head_count, width):
    base = jax.random.fold_in(key, tag)
    query_key, key_key = jax.random.split(base)
    queries = 1.3 * jax.random.normal(query_key, (TOKENS, head_count, width), jnp.float32)
    keys = 1.3 * jax.random.normal(key_key, (TOKENS, head_count, width), jnp.float32)
    return (queries.astype(jnp.bfloat16), keys.astype(jnp.bfloat16))


def draw_query_a(key, part):
    return drawn_pair(key, 11, HA, 2 * DA)[0]


def draw_key_a(key, part):
    return drawn_pair(key, 11, HA, 2 * DA)[1]


def draw_query_b(key, part):
    return drawn_pair(key, 23, HB, 2 * DB)[0]


def draw_key_b(key, part):
    return drawn_pair(key, 23, HB, 2 * DB)[1]


def steps_of(rng, extent, pieces, smallest, high):
    def one(axis_at, parts):
        heights = jax.random.uniform(jax.random.fold_in(jax.random.fold_in(rng, 6), axis_at), (parts,), jnp.float32, smallest / len(pieces), high / len(pieces))
        return jnp.repeat(jnp.exp(heights), extent[axis_at] // parts).reshape((-1,) + (1,) * (len(extent) - axis_at - 1))

    gain = one(*pieces[0])
    for cut in pieces[1:]:
        gain = gain * one(*cut)
    return gain


def shared_out(own_key, own, number, rows, amount, top, reach, slope):
    order = jax.random.permutation(own_key, amount)
    packed, usual = load_shares(amount, rows * top, reach, slope, True), load_shares(amount, rows * top, reach, slope, False)
    places = jnp.arange(amount)

    def named(sizes, turn):
        used = int((sizes > 0).sum())
        fixed = max(1, used // 4)
        passed = fixed + (places - fixed + turn * (used - fixed)) % max(1, amount - fixed)
        return jnp.zeros((amount,), jnp.int32).at[order[jnp.where(places < fixed, places, passed)]].set(jnp.asarray(sizes, jnp.int32))

    sizes = jnp.where(number % 4 == 0, named(packed, number // 4), named(usual, number - number // 4 - 1))
    mixed = jax.random.permutation(jax.random.fold_in(own, 3), amount)
    giver, sink = mixed[0:amount // 2 * 2:2], mixed[1:amount // 2 * 2:2]
    slack = jnp.minimum(sizes[giver] - 1, reach - sizes[sink]) // 2
    slack = jnp.where((giver == order[0]) | (sink == order[0]) | (sizes[sink] == 0), 0, jnp.maximum(slack, 0))
    passed = jax.random.randint(jax.random.fold_in(own, 4), (amount // 2,), 0, 1 << 20) % (slack + 1)
    sizes = sizes.at[giver].add(-passed).at[sink].add(passed)
    items = jnp.searchsorted(jnp.cumsum(sizes), jnp.arange(rows * top), side="right").astype(jnp.int32)
    grid = items.reshape(top, rows).T
    grid = grid[jax.random.permutation(jax.random.fold_in(own, 1), rows)]
    turn = jax.random.randint(jax.random.fold_in(own, 2), (rows, 1), 0, top)
    return jnp.take_along_axis(grid, (jnp.arange(top)[None, :] + turn) % top, axis=1)


def load_shares(number_of, total, limit, skew, full):
    portions = [(1 << 20) // math.isqrt(grade ** skew) + 1 for grade in range(1, number_of + 1)]
    largest = limit if full else min(limit, max(-(-total // number_of), total * portions[0] // sum(portions)))
    least = 1 if total - largest >= number_of - 1 else 0
    counts, rest = [largest] + [least] * (number_of - 1), total - largest - least * (number_of - 1)
    while rest > 0:
        free = [i for i in range(1, number_of) if counts[i] < largest] or [i for i in range(1, number_of) if counts[i] < limit]
        whole, remaining = sum([portions[i] for i in free]), rest
        for i in free:
            addition = min(limit - counts[i], max(1, remaining * portions[i] // whole), rest)
            counts[i] = counts[i] + addition
            rest = rest - addition
    return np.array(counts)


def noise(stream_key, extent, scale, reach, pieces=(), kind=jnp.bfloat16):
    values = jax.random.normal(stream_key, extent, jnp.float32) * scale
    if len(pieces) > 0:
        values = steps_of(stream_key, extent, pieces, -0.22, 0.18) * values
    return jnp.clip(values, min=-reach, max=reach).astype(kind)


def setup_inputs(seed: int = 0) -> dict:
    seeds = jax.random.split(jax.random.key(seed), 21)
    resid = noise(seeds[0], (TOKENS, D), 1.0, 6.0, ((0, 32),))
    query_a = draw_query_a(jax.random.fold_in(seeds[20], 71), 0)
    key_a = draw_key_a(jax.random.fold_in(seeds[20], 71), 0)
    value_a = noise(seeds[3], (TOKENS, HA, DV), 1.0, 6.0, ((0, 8), (1, 4)))
    query_b = draw_query_b(jax.random.fold_in(seeds[20], 71), 0)
    key_b = draw_key_b(jax.random.fold_in(seeds[20], 71), 0)
    value_b = noise(seeds[6], (TOKENS, HB, DV), 1.0, 6.0, ((0, 8), (1, 4)))
    lambda_a = jnp.clip(0.3 + 0.5 * jax.random.uniform(seeds[7], (HA,), jnp.float32) ** steps_of(seeds[7], (HA,), ((0, 4),), -0.2, 0.2), 0.3, 0.8)
    lambda_b = jnp.clip(0.3 + 0.5 * jax.random.uniform(seeds[8], (HB,), jnp.float32) ** steps_of(seeds[8], (HB,), ((0, 4),), -0.2, 0.2), 0.3, 0.8)
    head_gain = jnp.clip(1.0 + 0.18 * jax.random.normal(seeds[9], (DV,), jnp.float32), 0.1, 1.9)
    out_weight = noise(seeds[10], ((HA + HB) * DV, D), ((HA + HB) * DV) ** -0.5, 0.1875)
    norm_gain = jnp.clip(1.0 + 0.18 * jax.random.normal(seeds[11], (D,), jnp.float32), 0.1, 1.9)
    expert_ids_keys = jax.random.split(jax.random.fold_in(seeds[12], 1), TOKENS // TOK_DEV)
    expert_ids_turns = jax.random.permutation(jax.random.fold_in(seeds[12], 3), TOKENS // TOK_DEV)
    expert_ids = jax.vmap(lambda own, number: shared_out(jax.random.fold_in(seeds[12], 2), own, number, TOK_DEV, EXPERTS, TOPK, CAP, 2))(expert_ids_keys, expert_ids_turns).reshape((TOKENS, TOPK))
    expert_mix = jnp.clip(jnp.exp(math.log(1.0) - 1.609438 * jax.random.uniform(seeds[13], (TOKENS, TOPK), jnp.float32) ** steps_of(seeds[13], (TOKENS, TOPK), ((0, 32),), -0.2, 0.2)), 0.2, 1.0)
    gate_experts = noise(seeds[14], (EXPERTS, D, EFF), D ** -0.5, 0.125, ((0, 32),))
    up_experts = noise(seeds[15], (EXPERTS, D, EFF), D ** -0.5, 0.125, ((0, 32),))
    down_experts = noise(seeds[16], (EXPERTS, EFF, D), EFF ** -0.5, 0.1875, ((0, 32),))
    shared_gate = noise(seeds[17], (D, SFF), D ** -0.5, 0.125)
    shared_up = noise(seeds[18], (D, SFF), D ** -0.5, 0.125)
    shared_down = noise(seeds[19], (SFF, D), SFF ** -0.5, 0.25)
    return dict(resid=resid, query_a=query_a, key_a=key_a, value_a=value_a, query_b=query_b, key_b=key_b, value_b=value_b, lambda_a=lambda_a, lambda_b=lambda_b, head_gain=head_gain, out_weight=out_weight, norm_gain=norm_gain, expert_ids=expert_ids, expert_mix=expert_mix, gate_experts=gate_experts, up_experts=up_experts, down_experts=down_experts, shared_gate=shared_gate, shared_up=shared_up, shared_down=shared_down)


NEG_FILL = -1e+30
EPSILON = 1e-05
HEAD_SCALE = 0.8

def group_attention(queries, keys, values, lambdas, head_gain):
    seq_total = queries.shape[0]
    map_width = queries.shape[2] // 2
    head_count = queries.shape[1]
    value_width = values.shape[2]
    block_rows = min(512, seq_total)
    key_float = keys.astype(jnp.float32)
    value_float = values.astype(jnp.float32)
    key_pos = jnp.arange(seq_total, dtype=jnp.int32)
    scaling = map_width ** (-0.5)

    def one_block(begin_row):
        query_block = lax.dynamic_slice_in_dim(queries, begin_row, block_rows, 0).astype(jnp.float32)
        query_pos = begin_row + jnp.arange(block_rows, dtype=jnp.int32)
        causal = (key_pos[None, :] <= query_pos[:, None])[None]
        results = []
        for map_index in range(2):
            low_col = map_index * map_width
            scores = jnp.einsum('qhd,khd->hqk', query_block[:, :, low_col:low_col + map_width], key_float[:, :, low_col:low_col + map_width]) * scaling
            scores = jnp.where(causal, scores, NEG_FILL)
            row_top = lax.optimization_barrier(jnp.max(scores, axis=2, keepdims=True))
            exponent = jnp.where(causal, jnp.exp(scores - row_top), 0.0)
            denoms = lax.optimization_barrier(jnp.sum(exponent, axis=2))
            rounded = lax.optimization_barrier(exponent.astype(jnp.bfloat16)).astype(jnp.float32)
            numerator = jnp.einsum('hqk,khe->qhe', rounded, value_float)
            results.append(numerator / jnp.transpose(denoms)[:, :, None])
        differ = results[0] - lambdas[None, :, None] * results[1]
        scale_rms = lax.rsqrt(lax.optimization_barrier(jnp.mean(differ * differ, axis=2, keepdims=True)) + EPSILON)
        return (differ * scale_rms * head_gain[None, None, :] * HEAD_SCALE).astype(jnp.bfloat16)
    starts = jnp.arange(seq_total // block_rows, dtype=jnp.int32) * block_rows
    outputs = lax.map(one_block, starts)
    return outputs.reshape(seq_total, head_count, value_width)

def swiglu_rows(row_set, w_gate, w_up, w_down):
    gate_val = jnp.dot(row_set, w_gate, preferred_element_type=jnp.float32)
    up_val = jnp.dot(row_set, w_up, preferred_element_type=jnp.float32)
    hidden = (jax.nn.silu(gate_val) * up_val).astype(jnp.bfloat16)
    return jnp.dot(hidden, w_down, preferred_element_type=jnp.float32)

def reference(resid, query_a, key_a, value_a, query_b, key_b, value_b, lambda_a, lambda_b, head_gain, out_weight, norm_gain, expert_ids, expert_mix, gate_experts, up_experts, down_experts, shared_gate, shared_up, shared_down):
    seq_total = resid.shape[0]
    heads_a = group_attention(query_a, key_a, value_a, lambda_a, head_gain)
    heads_b = group_attention(query_b, key_b, value_b, lambda_b, head_gain)
    joined = jnp.concatenate([heads_a.reshape(seq_total, -1), heads_b.reshape(seq_total, -1)], axis=1)
    project = jnp.dot(joined, out_weight, preferred_element_type=jnp.float32)
    middle = (resid.astype(jnp.float32) + project).astype(jnp.bfloat16)
    middle_f = middle.astype(jnp.float32)
    normed = (middle_f * lax.rsqrt(lax.optimization_barrier(jnp.mean(middle_f * middle_f, axis=1, keepdims=True)) + EPSILON) * norm_gain[None, :]).astype(jnp.bfloat16)
    shared = swiglu_rows(normed, shared_gate, shared_up, shared_down)
    top_count = expert_ids.shape[1]
    flat_ids = expert_ids.reshape(-1).astype(jnp.int32)
    flat_mix = expert_mix.reshape(-1)
    expert_count = gate_experts.shape[0]
    sorted_pairs = jnp.argsort(flat_ids, stable=True).astype(jnp.int32)
    load_counts = lax.optimization_barrier(jnp.sum((flat_ids[:, None] == jnp.arange(expert_count, dtype=jnp.int32)[None, :]).astype(jnp.int32), axis=0))
    offsets = (jnp.cumsum(load_counts) - load_counts).astype(jnp.int32)
    most_rows = N_SP * N_TP * CAP
    padded_pairs = jnp.concatenate([sorted_pairs, jnp.zeros((most_rows,), jnp.int32)])

    def one_expert(routed, inputs):
        expert_index, w_gate, w_up, w_down = inputs
        picked = lax.dynamic_slice_in_dim(padded_pairs, offsets[expert_index], most_rows, 0)
        is_valid = jnp.arange(most_rows, dtype=jnp.int32) < load_counts[expert_index]
        token_rows = (picked // top_count).astype(jnp.int32)
        result = swiglu_rows(normed[token_rows], w_gate, w_up, w_down)
        result = lax.optimization_barrier(result.astype(jnp.bfloat16)).astype(jnp.float32)
        weights = jnp.where(is_valid, flat_mix[picked], 0.0)
        return (routed.at[token_rows].add(result * weights[:, None]), None)
    routed = lax.scan(one_expert, jnp.zeros((seq_total, D), jnp.float32), (jnp.arange(expert_count, dtype=jnp.int32), gate_experts, up_experts, down_experts))[0]
    return (middle_f + shared + routed).astype(jnp.bfloat16)
```

```python
import functools
import math

import jax
import jax.numpy as jnp
from jax import lax
from jax.experimental import pallas as pl
from jax.experimental.pallas import tpu as pltpu
from jax.sharding import PartitionSpec as P

NEG_FILL = -1e30
EPSILON = 1e-05
HEAD_SCALE = 0.8
MESH = pl.DeviceIdType.MESH


def swiglu_rows(row_set, w_gate, w_up, w_down):
    gate_val = jnp.dot(row_set, w_gate, preferred_element_type=jnp.float32)
    up_val = jnp.dot(row_set, w_up, preferred_element_type=jnp.float32)
    hidden = (jax.nn.silu(gate_val) * up_val).astype(jnp.bfloat16)
    return jnp.dot(hidden, w_down, preferred_element_type=jnp.float32)


def attention_kernel(
    sp_count,
    tp_count,
    scalings,
    query_a,
    query_b,
    local_a,
    local_b,
    lam_a,
    lam_b,
    gain,
    joined,
    kv_a,
    kv_b,
    tops,
    sums,
    numers,
    heads,
    send_z,
    send_y,
    recv,
    send_t,
    recv_t,
):
    sp = lax.axis_index("sp")
    tp = lax.axis_index("tp")
    chain = sp_count // 2
    spot = sp // 2
    side = sp % 2
    other = spot * 2 + (1 - side)
    rows = local_a.shape[0]
    part = rows // tp_count
    width = gain.shape[1]
    stores = (kv_a, kv_b)
    queries = (query_a, query_b)

    barrier = pltpu.get_barrier_semaphore()

    @pl.when(spot > 0)
    def _():
        pl.semaphore_signal(barrier, inc=1, device_id=(sp - 2, tp), device_id_type=MESH)

    @pl.when(spot < chain - 1)
    def _():
        pl.semaphore_signal(barrier, inc=1, device_id=(sp + 2, tp), device_id_type=MESH)

    pl.semaphore_signal(barrier, inc=1, device_id=(other, tp), device_id_type=MESH)
    for step in range(1, tp_count):
        peer = (tp + step) % tp_count
        pl.semaphore_signal(barrier, inc=1, device_id=(sp, peer), device_id_type=MESH)

    kv_a[sp] = local_a[...]
    kv_b[sp] = local_b[...]
    tops[...] = jnp.full(tops.shape, NEG_FILL, jnp.float32)
    sums[...] = jnp.zeros(sums.shape, jnp.float32)
    numers[...] = jnp.zeros(numers.shape, jnp.float32)
    linked = jnp.where(spot > 0, 1, 0) + jnp.where(spot < chain - 1, 1, 0) + tp_count
    pl.semaphore_wait(barrier, linked)

    def along(block, group, source):
        return pltpu.make_async_remote_copy(
            src_ref=source,
            dst_ref=stores[group].at[block],
            send_sem=send_z.at[block, group],
            recv_sem=recv.at[block, group],
            device_id=(sp + 2, tp),
            device_id_type=MESH,
        )

    def across(block, group, source):
        return pltpu.make_async_remote_copy(
            src_ref=source,
            dst_ref=stores[group].at[block],
            send_sem=send_y.at[block, group],
            recv_sem=recv.at[block, group],
            device_id=(other, tp),
            device_id_type=MESH,
        )

    def attend(block, group):
        store = stores[group]
        query = queries[group]
        key_width = store.shape[2] - width
        base = (sp - block) * rows
        row_at = lax.broadcasted_iota(jnp.int32, (rows, rows), 0)
        col_at = lax.broadcasted_iota(jnp.int32, (rows, rows), 1)
        causal = col_at <= row_at + base
        value = store[block, :, key_width:]
        for index in range(2):
            at = group * 2 + index
            if query.shape[2] == key_width:
                key = store[block, :, :key_width]
            else:
                half = key_width // 2
                key = store[block, :, index * half : (index + 1) * half]
            scores = (
                lax.dot_general(
                    query[index],
                    key,
                    (((1,), (1,)), ((), ())),
                    preferred_element_type=jnp.float32,
                )
                * scalings[group]
            )
            scores = jnp.where(causal, scores, NEG_FILL)
            old_top = tops[at][:, :1]
            new_top = jnp.maximum(old_top, jnp.max(scores, axis=1, keepdims=True))
            exponent = jnp.where(causal, jnp.exp(scores - new_top), 0.0)
            shrink = jnp.exp(old_top - new_top)
            total = sums[at][:, :1] * shrink + jnp.sum(exponent, axis=1, keepdims=True)
            tops[at] = jnp.broadcast_to(new_top, tops.shape[1:])
            sums[at] = jnp.broadcast_to(total, sums.shape[1:])
            numers[at] = numers[at] * shrink + jnp.dot(
                exponent.astype(jnp.bfloat16), value, preferred_element_type=jnp.float32
            )

    locals_ = (local_a, local_b)
    for group in range(2):

        @pl.when(spot < chain - 1)
        def _():
            along(sp, group, locals_[group]).start()

        @pl.when(side == 0)
        def _():
            across(sp, group, locals_[group]).start()

    for group in range(2):
        attend(sp, group)

    @pl.when(side == 1)
    def _():
        for group in range(2):
            across(other, group, stores[group].at[other]).wait_recv()
            attend(other, group)

    @pl.loop(1, chain)
    def _(back):
        @pl.when(back <= spot)
        def _():
            mine = sp - 2 * back
            theirs = other - 2 * back
            for group in range(2):
                along(mine, group, stores[group].at[mine]).wait_recv()

                @pl.when(spot < chain - 1)
                def _():
                    along(mine, group, stores[group].at[mine]).start()

                across(mine, group, stores[group].at[mine]).start()
            for group in range(2):
                attend(mine, group)
            for group in range(2):
                across(theirs, group, stores[group].at[theirs]).wait_recv()
                attend(theirs, group)

    lams = (lam_a, lam_b)
    for group in range(2):
        first = numers[2 * group] / sums[2 * group][:, :1]
        second = numers[2 * group + 1] / sums[2 * group + 1][:, :1]
        differ = first - lams[group][0] * second
        scale_rms = lax.rsqrt(jnp.mean(differ * differ, axis=1, keepdims=True) + EPSILON)
        heads[:, group * width : (group + 1) * width] = (
            differ * scale_rms * gain[...] * HEAD_SCALE
        ).astype(jnp.bfloat16)

    def columns(who, group):
        return pl.ds(pl.multiple_of((group * tp_count + who) * width, width), width)

    def spread(step, group):
        peer = (tp + step) % tp_count
        start = pl.multiple_of(peer * part, part)
        return pltpu.make_async_remote_copy(
            src_ref=heads.at[pl.ds(start, part), group * width : (group + 1) * width],
            dst_ref=joined.at[:, columns(tp, group)],
            send_sem=send_t.at[step, group],
            recv_sem=recv_t.at[step, group],
            device_id=(sp, peer),
            device_id_type=MESH,
        )

    for step in range(1, tp_count):
        for group in range(2):
            spread(step, group).start()
    own = pl.multiple_of(tp * part, part)
    for group in range(2):
        joined[:, columns(tp, group)] = heads[
            pl.ds(own, part), group * width : (group + 1) * width
        ]

    for group in range(2):

        @pl.when(spot < chain - 1)
        def _():
            along(sp, group, locals_[group]).wait_send()

        @pl.when(side == 0)
        def _():
            across(sp, group, locals_[group]).wait_send()

    @pl.loop(1, chain)
    def _(back):
        @pl.when(back <= spot)
        def _():
            mine = sp - 2 * back
            for group in range(2):

                @pl.when(spot < chain - 1)
                def _():
                    along(mine, group, stores[group].at[mine]).wait_send()

                across(mine, group, stores[group].at[mine]).wait_send()

    for step in range(1, tp_count):
        for group in range(2):
            spread(step, group).wait()


def attention(
    query_a, key_a, value_a, query_b, key_b, value_b, lambda_a, lambda_b, head_gain
):
    sp_count = lax.axis_size("sp")
    tp_count = lax.axis_size("tp")
    rows = query_a.shape[0]
    width = value_a.shape[2]

    def maps_of(query):
        flat = query[:, 0]
        size = flat.shape[1] // 2
        if size % 128 == 0:
            return jnp.stack([flat[:, :size], flat[:, size:]])
        first = jnp.arange(2 * size) < size
        zero = jnp.zeros_like(flat)
        return jnp.stack([jnp.where(first, flat, zero), jnp.where(first, zero, flat)])

    local_a = jnp.concatenate([key_a[:, 0], value_a[:, 0]], axis=1)
    local_b = jnp.concatenate([key_b[:, 0], value_b[:, 0]], axis=1)
    scalings = ((query_a.shape[2] // 2) ** (-0.5), (query_b.shape[2] // 2) ** (-0.5))
    vmem = pl.BlockSpec(memory_space=pltpu.VMEM)
    smem = pl.BlockSpec(memory_space=pltpu.SMEM)
    dma = pltpu.SemaphoreType.DMA
    return pl.pallas_call(
        functools.partial(attention_kernel, sp_count, tp_count, scalings),
        out_shape=jax.ShapeDtypeStruct((rows // tp_count, 2 * tp_count * width), jnp.bfloat16),
        in_specs=[vmem, vmem, vmem, vmem, smem, smem, vmem],
        out_specs=vmem,
        scratch_shapes=[
            pltpu.VMEM((sp_count,) + local_a.shape, jnp.bfloat16),
            pltpu.VMEM((sp_count,) + local_b.shape, jnp.bfloat16),
            pltpu.VMEM((4, rows, 128), jnp.float32),
            pltpu.VMEM((4, rows, 128), jnp.float32),
            pltpu.VMEM((4, rows, width), jnp.float32),
            pltpu.VMEM((rows, 2 * width), jnp.bfloat16),
            dma((sp_count, 2)),
            dma((sp_count, 2)),
            dma((sp_count, 2)),
            dma((tp_count, 2)),
            dma((tp_count, 2)),
        ],
        compiler_params=pltpu.CompilerParams(collective_id=0, has_side_effects=True),
        name="attention",
    )(
        maps_of(query_a),
        maps_of(query_b),
        local_a,
        local_b,
        lambda_a,
        lambda_b,
        head_gain[None, :],
    )


def per_device(
    resid,
    query_a,
    key_a,
    value_a,
    query_b,
    key_b,
    value_b,
    lambda_a,
    lambda_b,
    head_gain,
    out_weight,
    norm_gain,
    expert_ids,
    expert_mix,
    gate_experts,
    up_experts,
    down_experts,
    shared_gate,
    shared_up,
    shared_down,
):
    tok_dev = resid.shape[0]
    joined = attention(
        query_a, key_a, value_a, query_b, key_b, value_b, lambda_a, lambda_b, head_gain
    )
    project = jnp.dot(joined, out_weight, preferred_element_type=jnp.float32)
    middle = (resid.astype(jnp.float32) + project).astype(jnp.bfloat16)
    middle_f = middle.astype(jnp.float32)
    normed = (
        middle_f
        * lax.rsqrt(jnp.mean(middle_f * middle_f, axis=1, keepdims=True) + EPSILON)
        * norm_gain[None, :]
    ).astype(jnp.bfloat16)
    shared = swiglu_rows(normed, shared_gate, shared_up, shared_down)
    top_count = expert_ids.shape[1]
    model_width = normed.shape[1]
    sp_count = lax.axis_size("sp")
    tp_count = lax.axis_size("tp")
    expert_total = sp_count * tp_count
    pair_count = tok_dev * top_count
    capacity = max(2, 2 * pair_count // expert_total)
    hits = expert_ids[:, :, None] == jnp.arange(expert_total, dtype=jnp.int32)[None, None, :]
    named = jnp.any(hits, axis=1)
    mix_dense = jnp.sum(jnp.where(hits, expert_mix[:, :, None], 0.0), axis=1)
    counted = named.astype(jnp.int32)
    ranks = jnp.where(named, jnp.cumsum(counted, axis=0) - counted, -1)
    slots = jnp.arange(capacity, dtype=jnp.int32)
    placing = (ranks[:, :, None] == slots[None, None, :]).reshape(tok_dev, -1)
    send_rows = lax.dot_general(
        placing.astype(jnp.bfloat16),
        normed,
        (((0,), (0,)), ((), ())),
        preferred_element_type=jnp.float32,
    ).astype(jnp.bfloat16)
    send_rows = send_rows.reshape(expert_total, capacity, model_width)
    arrived = lax.all_to_all(send_rows, ("sp", "tp"), split_axis=0, concat_axis=0, tiled=True)
    arrived_shape = arrived.shape
    flat_rows = arrived.reshape(-1, arrived_shape[-1])
    result = swiglu_rows(flat_rows, gate_experts[0], up_experts[0], down_experts[0]).astype(
        jnp.bfloat16
    )
    finished = result.reshape(arrived_shape)
    returned = lax.all_to_all(finished, ("sp", "tp"), split_axis=0, concat_axis=0, tiled=True)
    flat_mix = jnp.broadcast_to(mix_dense[:, :, None], ranks.shape + (capacity,))
    weights = jnp.where(placing, flat_mix.reshape(tok_dev, -1), 0.0)
    coarse = lax.reduce_precision(weights, 8, 7)
    fine = weights - coarse
    flat_back = returned.reshape(-1, model_width)
    both = jnp.dot(
        jnp.concatenate([coarse, fine], axis=0).astype(jnp.bfloat16),
        flat_back,
        preferred_element_type=jnp.float32,
    )
    routed = both[:tok_dev] + both[tok_dev:]
    return (middle_f + shared + routed).astype(jnp.bfloat16)


def solution(mesh):
    in_specs = (
        P(("sp", "tp"), None),
        P("sp", "tp", None),
        P("sp", "tp", None),
        P("sp", "tp", None),
        P("sp", "tp", None),
        P("sp", "tp", None),
        P("sp", "tp", None),
        P("tp"),
        P("tp"),
        P(),
        P(),
        P(),
        P(("sp", "tp"), None),
        P(("sp", "tp"), None),
        P(("sp", "tp"), None, None),
        P(("sp", "tp"), None, None),
        P(("sp", "tp"), None, None),
        P(),
        P(),
        P(),
    )
    out_specs = P(("sp", "tp"), None)
    return jax.shard_map(
        per_device, mesh=mesh, in_specs=in_specs, out_specs=out_specs, check_vma=False
    )
```

```python
import functools
import math

import jax
import jax.numpy as jnp
from jax import lax
from jax.experimental import pallas as pl
from jax.experimental.pallas import tpu as pltpu
from jax.sharding import PartitionSpec as P

NEG_FILL = -1e30
EPSILON = 1e-05
HEAD_SCALE = 0.8
MESH = pl.DeviceIdType.MESH


def swiglu_rows(row_set, w_gate, w_up, w_down):
    gate_val = jnp.dot(row_set, w_gate, preferred_element_type=jnp.float32)
    up_val = jnp.dot(row_set, w_up, preferred_element_type=jnp.float32)
    hidden = (jax.nn.silu(gate_val) * up_val).astype(jnp.bfloat16)
    return jnp.dot(hidden, w_down, preferred_element_type=jnp.float32)


def attention_kernel(
    sp_count,
    tp_count,
    scalings,
    query_a,
    query_b,
    local_a,
    local_b,
    lam_a,
    lam_b,
    gain,
    joined,
    kv_a,
    kv_b,
    tops,
    sums,
    numers,
    heads,
    send_z,
    send_y,
    recv,
    send_t,
    recv_t,
):
    sp = lax.axis_index("sp")
    tp = lax.axis_index("tp")
    chain = sp_count // 2
    spot = sp // 2
    side = sp % 2
    other = spot * 2 + (1 - side)
    rows = local_a.shape[0]
    part = rows // tp_count
    width = gain.shape[1]
    stores = (kv_a, kv_b)
    queries = (query_a, query_b)

    barrier = pltpu.get_barrier_semaphore()

    @pl.when(spot > 0)
    def _():
        pl.semaphore_signal(barrier, inc=1, device_id=(sp - 2, tp), device_id_type=MESH)

    @pl.when(spot < chain - 1)
    def _():
        pl.semaphore_signal(barrier, inc=1, device_id=(sp + 2, tp), device_id_type=MESH)

    pl.semaphore_signal(barrier, inc=1, device_id=(other, tp), device_id_type=MESH)
    for step in range(1, tp_count):
        peer = (tp + step) % tp_count
        pl.semaphore_signal(barrier, inc=1, device_id=(sp, peer), device_id_type=MESH)

    kv_a[sp] = local_a[...]
    kv_b[sp] = local_b[...]
    tops[...] = jnp.full(tops.shape, NEG_FILL, jnp.float32)
    sums[...] = jnp.zeros(sums.shape, jnp.float32)
    numers[...] = jnp.zeros(numers.shape, jnp.float32)
    linked = jnp.where(spot > 0, 1, 0) + jnp.where(spot < chain - 1, 1, 0) + tp_count
    pl.semaphore_wait(barrier, linked)

    def along(block, group, source):
        return pltpu.make_async_remote_copy(
            src_ref=source,
            dst_ref=stores[group].at[block],
            send_sem=send_z.at[block, group],
            recv_sem=recv.at[block, group],
            device_id=(sp + 2, tp),
            device_id_type=MESH,
        )

    def across(block, group, source):
        return pltpu.make_async_remote_copy(
            src_ref=source,
            dst_ref=stores[group].at[block],
            send_sem=send_y.at[block, group],
            recv_sem=recv.at[block, group],
            device_id=(other, tp),
            device_id_type=MESH,
        )

    def attend(block, group):
        store = stores[group]
        query = queries[group]
        key_width = store.shape[2] - width
        base = (sp - block) * rows
        row_at = lax.broadcasted_iota(jnp.int32, (rows, rows), 0)
        col_at = lax.broadcasted_iota(jnp.int32, (rows, rows), 1)
        causal = col_at <= row_at + base
        value = store[block, :, key_width:]
        for index in range(2):
            at = group * 2 + index
            if query.shape[2] == key_width:
                key = store[block, :, :key_width]
            else:
                half = key_width // 2
                key = store[block, :, index * half : (index + 1) * half]
            scores = (
                lax.dot_general(
                    query[index],
                    key,
                    (((1,), (1,)), ((), ())),
                    preferred_element_type=jnp.float32,
                )
                * scalings[group]
            )
            scores = jnp.where(causal, scores, NEG_FILL)
            old_top = tops[at][:, :1]
            new_top = jnp.maximum(old_top, jnp.max(scores, axis=1, keepdims=True))
            exponent = jnp.where(causal, jnp.exp(scores - new_top), 0.0)
            shrink = jnp.exp(old_top - new_top)
            total = sums[at][:, :1] * shrink + jnp.sum(exponent, axis=1, keepdims=True)
            tops[at] = jnp.broadcast_to(new_top, tops.shape[1:])
            sums[at] = jnp.broadcast_to(total, sums.shape[1:])
            numers[at] = numers[at] * shrink + jnp.dot(
                exponent.astype(jnp.bfloat16), value, preferred_element_type=jnp.float32
            )

    locals_ = (local_a, local_b)
    for group in range(2):

        @pl.when(spot < chain - 1)
        def _():
            along(sp, group, locals_[group]).start()

        @pl.when(side == 0)
        def _():
            across(sp, group, locals_[group]).start()

    for group in range(2):
        attend(sp, group)

    @pl.when(side == 1)
    def _():
        for group in range(2):
            across(other, group, stores[group].at[other]).wait_recv()
            attend(other, group)

    @pl.loop(1, chain)
    def _(back):
        @pl.when(back <= spot)
        def _():
            mine = sp - 2 * back
            theirs = other - 2 * back
            for group in range(2):
                along(mine, group, stores[group].at[mine]).wait_recv()

                @pl.when(spot < chain - 1)
                def _():
                    along(mine, group, stores[group].at[mine]).start()

                across(mine, group, stores[group].at[mine]).start()
            for group in range(2):
                attend(mine, group)
            for group in range(2):
                across(theirs, group, stores[group].at[theirs]).wait_recv()
                attend(theirs, group)

    lams = (lam_a, lam_b)
    for group in range(2):
        first = numers[2 * group] / sums[2 * group][:, :1]
        second = numers[2 * group + 1] / sums[2 * group + 1][:, :1]
        differ = first - lams[group][0] * second
        scale_rms = lax.rsqrt(jnp.mean(differ * differ, axis=1, keepdims=True) + EPSILON)
        heads[:, group * width : (group + 1) * width] = (
            differ * scale_rms * gain[...] * HEAD_SCALE
        ).astype(jnp.bfloat16)

    def columns(who, group):
        return pl.ds(pl.multiple_of((group * tp_count + who) * width, width), width)

    def spread(step, group):
        peer = (tp + step) % tp_count
        start = pl.multiple_of(peer * part, part)
        return pltpu.make_async_remote_copy(
            src_ref=heads.at[pl.ds(start, part), group * width : (group + 1) * width],
            dst_ref=joined.at[:, columns(tp, group)],
            send_sem=send_t.at[step, group],
            recv_sem=recv_t.at[step, group],
            device_id=(sp, peer),
            device_id_type=MESH,
        )

    for step in range(1, tp_count):
        for group in range(2):
            spread(step, group).start()
    own = pl.multiple_of(tp * part, part)
    for group in range(2):
        joined[:, columns(tp, group)] = heads[
            pl.ds(own, part), group * width : (group + 1) * width
        ]

    for group in range(2):

        @pl.when(spot < chain - 1)
        def _():
            along(sp, group, locals_[group]).wait_send()

        @pl.when(side == 0)
        def _():
            across(sp, group, locals_[group]).wait_send()

    @pl.loop(1, chain)
    def _(back):
        @pl.when(back <= spot)
        def _():
            mine = sp - 2 * back
            for group in range(2):

                @pl.when(spot < chain - 1)
                def _():
                    along(mine, group, stores[group].at[mine]).wait_send()

                across(mine, group, stores[group].at[mine]).wait_send()

    for step in range(1, tp_count):
        for group in range(2):
            spread(step, group).wait()


def attention(
    query_a, key_a, value_a, query_b, key_b, value_b, lambda_a, lambda_b, head_gain
):
    sp_count = lax.axis_size("sp")
    tp_count = lax.axis_size("tp")
    rows = query_a.shape[0]
    width = value_a.shape[2]

    def maps_of(query):
        flat = query[:, 0]
        size = flat.shape[1] // 2
        if size % 128 == 0:
            return jnp.stack([flat[:, :size], flat[:, size:]])
        first = jnp.arange(2 * size) < size
        zero = jnp.zeros_like(flat)
        return jnp.stack([jnp.where(first, flat, zero), jnp.where(first, zero, flat)])

    local_a = jnp.concatenate([key_a[:, 0], value_a[:, 0]], axis=1)
    local_b = jnp.concatenate([key_b[:, 0], value_b[:, 0]], axis=1)
    scalings = ((query_a.shape[2] // 2) ** (-0.5), (query_b.shape[2] // 2) ** (-0.5))
    vmem = pl.BlockSpec(memory_space=pltpu.VMEM)
    smem = pl.BlockSpec(memory_space=pltpu.SMEM)
    dma = pltpu.SemaphoreType.DMA
    return pl.pallas_call(
        functools.partial(attention_kernel, sp_count, tp_count, scalings),
        out_shape=jax.ShapeDtypeStruct((rows // tp_count, 2 * tp_count * width), jnp.bfloat16),
        in_specs=[vmem, vmem, vmem, vmem, smem, smem, vmem],
        out_specs=vmem,
        scratch_shapes=[
            pltpu.VMEM((sp_count,) + local_a.shape, jnp.bfloat16),
            pltpu.VMEM((sp_count,) + local_b.shape, jnp.bfloat16),
            pltpu.VMEM((4, rows, 128), jnp.float32),
            pltpu.VMEM((4, rows, 128), jnp.float32),
            pltpu.VMEM((4, rows, width), jnp.float32),
            pltpu.VMEM((rows, 2 * width), jnp.bfloat16),
            dma((sp_count, 2)),
            dma((sp_count, 2)),
            dma((sp_count, 2)),
            dma((tp_count, 2)),
            dma((tp_count, 2)),
        ],
        compiler_params=pltpu.CompilerParams(collective_id=0, has_side_effects=True),
        name="attention",
    )(
        maps_of(query_a),
        maps_of(query_b),
        local_a,
        local_b,
        lambda_a,
        lambda_b,
        head_gain[None, :],
    )


def plane_device(spot, member, tp_count):
    return (spot * 2 + member // tp_count, member % tp_count)


def expand_lanes(meta, first, members, capacity):
    shape = (meta.shape[1], members * capacity)
    column = lax.broadcasted_iota(jnp.int32, shape, 0)
    lane = lax.broadcasted_iota(jnp.int32, shape, 1)
    gap = lane - (column - first) * capacity
    chosen = jnp.where((gap >= 0) & (gap < capacity), 1.0, 0.0).astype(jnp.bfloat16)
    return jnp.dot(meta, chosen, preferred_element_type=jnp.float32)


def dispatch_kernel(
    sp_count,
    tp_count,
    model_width,
    packed,
    slot_at,
    arrived,
    metas,
    held,
    picks,
    send_up,
    send_down,
    recv_z,
    send_p,
    recv_p,
):
    sp = lax.axis_index("sp")
    tp = lax.axis_index("tp")
    chain = sp_count // 2
    members = 2 * tp_count
    spot = sp // 2
    member = (sp % 2) * tp_count + tp
    capacity = arrived.shape[2]

    barrier = pltpu.get_barrier_semaphore()

    @pl.when(spot > 0)
    def _():
        pl.semaphore_signal(barrier, inc=1, device_id=(sp - 2, tp), device_id_type=MESH)

    @pl.when(spot < chain - 1)
    def _():
        pl.semaphore_signal(barrier, inc=1, device_id=(sp + 2, tp), device_id_type=MESH)

    for step in range(1, members):
        peer = plane_device(spot, (member + step) % members, tp_count)
        pl.semaphore_signal(barrier, inc=1, device_id=peer, device_id_type=MESH)
    linked = jnp.where(spot > 0, 1, 0) + jnp.where(spot < chain - 1, 1, 0) + members - 1
    pl.semaphore_wait(barrier, linked)

    def move(block, source, shift, sems):
        return pltpu.make_async_remote_copy(
            src_ref=source,
            dst_ref=held.at[block],
            send_sem=sems.at[block],
            recv_sem=recv_z.at[block],
            device_id=(sp + 2 * shift, tp),
            device_id_type=MESH,
        )

    def spread(block, step):
        target = (member + step) % members
        return pltpu.make_async_remote_copy(
            src_ref=picks.at[block, target],
            dst_ref=arrived.at[block, member],
            send_sem=send_p.at[block, step],
            recv_sem=recv_p.at[block, step],
            device_id=plane_device(spot, target, tp_count),
            device_id_type=MESH,
        )

    def place(block, source):
        meta = source[:, model_width:]
        metas[block] = meta
        ranks = expand_lanes(meta, spot * members, members, capacity)
        placing = jnp.where(ranks == slot_at[...], 1.0, 0.0).astype(jnp.bfloat16)
        rows = lax.dot_general(
            placing,
            source[:, :model_width],
            (((0,), (0,)), ((), ())),
            preferred_element_type=jnp.float32,
        )
        for index in range(members):
            picks[block, index] = rows[index * capacity : (index + 1) * capacity].astype(
                jnp.bfloat16
            )
        for step in range(1, members):
            spread(block, step).start()
        arrived[block, member] = picks[block, member]

    @pl.when(spot < chain - 1)
    def _():
        move(spot, packed, 1, send_up).start()

    @pl.when(spot > 0)
    def _():
        move(spot, packed, -1, send_down).start()

    place(spot, packed)

    @pl.loop(1, chain)
    def _(back):
        low = spot - back
        high = spot + back

        @pl.when(low >= 0)
        def _():
            move(low, held.at[low], 1, send_up).wait_recv()

            @pl.when(spot < chain - 1)
            def _():
                move(low, held.at[low], 1, send_up).start()

        @pl.when(high < chain)
        def _():
            move(high, held.at[high], -1, send_down).wait_recv()

            @pl.when(spot > 0)
            def _():
                move(high, held.at[high], -1, send_down).start()

        @pl.when(low >= 0)
        def _():
            place(low, held.at[low])

        @pl.when(high < chain)
        def _():
            place(high, held.at[high])

    @pl.when(spot < chain - 1)
    def _():
        move(spot, packed, 1, send_up).wait_send()

    @pl.when(spot > 0)
    def _():
        move(spot, packed, -1, send_down).wait_send()

    @pl.loop(1, chain)
    def _(back):
        low = spot - back
        high = spot + back

        @pl.when((low >= 0) & (spot < chain - 1))
        def _():
            move(low, held.at[low], 1, send_up).wait_send()

        @pl.when((high < chain) & (spot > 0))
        def _():
            move(high, held.at[high], -1, send_down).wait_send()

    @pl.loop(0, chain)
    def _(block):
        for step in range(1, members):
            spread(block, step).wait()


def return_kernel(
    sp_count,
    tp_count,
    expert_total,
    finished,
    metas,
    slot_at,
    middle,
    normed,
    gate,
    up,
    down,
    out,
    back,
    part_out,
    part_in,
    total,
    send_p,
    recv_p,
    send_z,
    recv_z,
):
    sp = lax.axis_index("sp")
    tp = lax.axis_index("tp")
    chain = sp_count // 2
    members = 2 * tp_count
    spot = sp // 2
    side = sp % 2
    member = side * tp_count + tp
    capacity = finished.shape[2]

    barrier = pltpu.get_barrier_semaphore()
    for step in range(1, members):
        peer = plane_device(spot, (member + step) % members, tp_count)
        pl.semaphore_signal(barrier, inc=1, device_id=peer, device_id_type=MESH)
    for step in range(1, chain):
        peer = (((spot + step) % chain) * 2 + side, tp)
        pl.semaphore_signal(barrier, inc=1, device_id=peer, device_id_type=MESH)
    pl.semaphore_wait(barrier, members + chain - 2)

    def spread(block, step):
        target = (member + step) % members
        return pltpu.make_async_remote_copy(
            src_ref=finished.at[block, target],
            dst_ref=back.at[block, member],
            send_sem=send_p.at[block, step],
            recv_sem=recv_p.at[block, step],
            device_id=plane_device(spot, target, tp_count),
            device_id_type=MESH,
        )

    def deliver(block):
        return pltpu.make_async_remote_copy(
            src_ref=part_out.at[block],
            dst_ref=part_in.at[spot],
            send_sem=send_z.at[block],
            recv_sem=recv_z.at[spot],
            device_id=(block * 2 + side, tp),
            device_id_type=MESH,
        )

    def collect(block):
        return pltpu.make_async_remote_copy(
            src_ref=part_out.at[block],
            dst_ref=part_in.at[block],
            send_sem=send_z.at[block],
            recv_sem=recv_z.at[block],
            device_id=(block * 2 + side, tp),
            device_id_type=MESH,
        )

    def far_first(body):
        @pl.loop(0, 2 * chain)
        def _(turn):
            away = chain - 1 - turn // 2
            block = spot + away * (1 - 2 * (turn % 2))

            @pl.when((block >= 0) & (block < chain) & ((away > 0) | (turn % 2 == 0)))
            def _():
                body(block)

    def start_spread(block):
        for step in range(1, members):
            spread(block, step).start()
        back[block, member] = finished[block, member]

    far_first(start_spread)

    rows = normed[...]
    gate_val = jnp.dot(rows, gate[...], preferred_element_type=jnp.float32)
    up_val = jnp.dot(rows, up[...], preferred_element_type=jnp.float32)
    hidden = (jax.nn.silu(gate_val) * up_val).astype(jnp.bfloat16)
    total[...] = middle[...].astype(jnp.float32) + jnp.dot(
        hidden, down[...], preferred_element_type=jnp.float32
    )

    def mix(block):
        for step in range(1, members):
            spread(block, step).wait_recv()
        meta = metas[block]
        first = spot * members
        ranks = expand_lanes(meta, first, members, capacity)
        coarse = expand_lanes(meta, first + expert_total, members, capacity)
        fine = expand_lanes(meta, first + 2 * expert_total, members, capacity)
        placed = ranks == slot_at[...]
        weights = jnp.concatenate(
            [jnp.where(placed, coarse, 0.0), jnp.where(placed, fine, 0.0)], axis=0
        ).astype(jnp.bfloat16)
        if capacity % 16 == 0:
            slots = back[block].reshape(members * capacity, back.shape[3])
        else:
            slots = jnp.concatenate(
                [back[block, index].astype(jnp.float32) for index in range(members)], axis=0
            ).astype(jnp.bfloat16)
        both = jnp.dot(weights, slots, preferred_element_type=jnp.float32)
        tokens = meta.shape[0]
        sums = both[:tokens] + both[tokens:]

        @pl.when(block == spot)
        def _():
            total[...] += sums

        @pl.when(block != spot)
        def _():
            part_out[block] = sums.astype(jnp.bfloat16)
            deliver(block).start()

    far_first(mix)

    @pl.loop(1, chain)
    def _(step):
        block = (spot + step) % chain
        collect(block).wait_recv()
        total[...] += part_in[block].astype(jnp.float32)

    out[...] = total[...].astype(jnp.bfloat16)

    @pl.loop(1, chain)
    def _(step):
        block = (spot + step) % chain
        deliver(block).wait_send()

    @pl.loop(0, chain)
    def _(block):
        for step in range(1, members):
            spread(block, step).wait_send()


def per_device(
    resid,
    query_a,
    key_a,
    value_a,
    query_b,
    key_b,
    value_b,
    lambda_a,
    lambda_b,
    head_gain,
    out_weight,
    norm_gain,
    expert_ids,
    expert_mix,
    gate_experts,
    up_experts,
    down_experts,
    shared_gate,
    shared_up,
    shared_down,
):
    tok_dev = resid.shape[0]
    joined = attention(
        query_a, key_a, value_a, query_b, key_b, value_b, lambda_a, lambda_b, head_gain
    )
    project = jnp.dot(joined, out_weight, preferred_element_type=jnp.float32)
    middle = (resid.astype(jnp.float32) + project).astype(jnp.bfloat16)
    middle_f = middle.astype(jnp.float32)
    normed = (
        middle_f
        * lax.rsqrt(jnp.mean(middle_f * middle_f, axis=1, keepdims=True) + EPSILON)
        * norm_gain[None, :]
    ).astype(jnp.bfloat16)
    top_count = expert_ids.shape[1]
    model_width = normed.shape[1]
    sp_count = lax.axis_size("sp")
    tp_count = lax.axis_size("tp")
    expert_total = sp_count * tp_count
    pair_count = tok_dev * top_count
    capacity = max(2, 2 * pair_count // expert_total)
    hits = expert_ids[:, :, None] == jnp.arange(expert_total, dtype=jnp.int32)[None, None, :]
    named = jnp.any(hits, axis=1)
    mix_dense = jnp.sum(jnp.where(hits, expert_mix[:, :, None], 0.0), axis=1)
    counted = named.astype(jnp.int32)
    ranks = jnp.where(named, jnp.cumsum(counted, axis=0) - counted, -1)
    coarse = lax.reduce_precision(mix_dense, 8, 7)
    meta = jnp.concatenate([ranks.astype(jnp.float32), coarse, mix_dense - coarse], axis=1)
    spare = -meta.shape[1] % 128
    meta = jnp.pad(meta, ((0, 0), (0, spare))).astype(jnp.bfloat16)
    packed = jnp.concatenate([normed, meta], axis=1)
    members = 2 * tp_count
    chain = sp_count // 2
    slot_at = jnp.tile(jnp.arange(capacity, dtype=jnp.float32), members)[None, :]
    vmem = pl.BlockSpec(memory_space=pltpu.VMEM)
    dma = pltpu.SemaphoreType.DMA
    slot_shape = (chain, members, capacity, model_width)
    arrived, metas = pl.pallas_call(
        functools.partial(dispatch_kernel, sp_count, tp_count, model_width),
        out_shape=(
            jax.ShapeDtypeStruct(slot_shape, jnp.bfloat16),
            jax.ShapeDtypeStruct((chain,) + meta.shape, jnp.bfloat16),
        ),
        in_specs=[vmem, vmem],
        out_specs=(vmem, vmem),
        scratch_shapes=[
            pltpu.VMEM((chain,) + packed.shape, jnp.bfloat16),
            pltpu.VMEM(slot_shape, jnp.bfloat16),
            dma((chain,)),
            dma((chain,)),
            dma((chain,)),
            dma((chain, members)),
            dma((chain, members)),
        ],
        compiler_params=pltpu.CompilerParams(collective_id=1, has_side_effects=True),
        name="dispatch",
    )(packed, slot_at)
    flat_rows = arrived.reshape(-1, model_width)
    result = swiglu_rows(flat_rows, gate_experts[0], up_experts[0], down_experts[0]).astype(
        jnp.bfloat16
    )
    return pl.pallas_call(
        functools.partial(return_kernel, sp_count, tp_count, expert_total),
        out_shape=jax.ShapeDtypeStruct((tok_dev, model_width), jnp.bfloat16),
        in_specs=[vmem] * 8,
        out_specs=vmem,
        scratch_shapes=[
            pltpu.VMEM(slot_shape, jnp.bfloat16),
            pltpu.VMEM((chain, tok_dev, model_width), jnp.bfloat16),
            pltpu.VMEM((chain, tok_dev, model_width), jnp.bfloat16),
            pltpu.VMEM((tok_dev, model_width), jnp.float32),
            dma((chain, members)),
            dma((chain, members)),
            dma((chain,)),
            dma((chain,)),
        ],
        compiler_params=pltpu.CompilerParams(collective_id=2, has_side_effects=True),
        name="give_back",
    )(
        result.reshape(slot_shape),
        metas,
        slot_at,
        middle,
        normed,
        shared_gate,
        shared_up,
        shared_down,
    )


def solution(mesh):
    in_specs = (
        P(("sp", "tp"), None),
        P("sp", "tp", None),
        P("sp", "tp", None),
        P("sp", "tp", None),
        P("sp", "tp", None),
        P("sp", "tp", None),
        P("sp", "tp", None),
        P("tp"),
        P("tp"),
        P(),
        P(),
        P(),
        P(("sp", "tp"), None),
        P(("sp", "tp"), None),
        P(("sp", "tp"), None, None),
        P(("sp", "tp"), None, None),
        P(("sp", "tp"), None, None),
        P(),
        P(),
        P(),
    )
    out_specs = P(("sp", "tp"), None)
    return jax.shard_map(
        per_device, mesh=mesh, in_specs=in_specs, out_specs=out_specs, check_vma=False
    )
```
